32 devices in a mesh: ep: 8 (over z, y), tp: 4 (over x, core).
Axes of the slice: x: 2, y: 2, z: 4, core: 2. Of those that a mesh axis runs over, the one named last changes fastest.
Arguments:
- queries: bfloat16 [2048, 8, 128], P('ep', 'tp'), may hold values from -15 to 15
- keys: bfloat16 [2048, 4, 128], P('ep', 'tp'), may hold values from -6 to 6
- values: bfloat16 [2048, 4, 128], P('ep', 'tp'), may hold values from -6 to 6
- key_bias: bfloat16 [2048, 8], P('ep', 'tp'), may hold values from -20 to 2
- out_weight: bfloat16 [1024, 2048], P('tp'), may hold values from -0.1875 to 0.1875
- tokens_b: bfloat16 [4096, 2048], P(('ep', 'tp')), may hold values from -6 to 6
- moe_gain: bfloat16 [2048], replicated, may hold values from 0.099609375 to 1.8984375
- gate_weight: bfloat16 [8, 2048, 2048], P('ep', None, 'tp'), may hold values from -0.125 to 0.125
- up_weight: bfloat16 [8, 2048, 2048], P('ep', None, 'tp'), may hold values from -0.125 to 0.125
- down_weight: bfloat16 [8, 2048, 2048], P('ep', 'tp'), may hold values from -0.125 to 0.125
- routes: int32 [4096, 2], P(('ep', 'tp')), may hold values from 0 to 7, all different within a row; in each aligned block of 128 rows (0 to 127, 128 to 255, ...) at most 48 rows name the same one
- route_weights: float32 [4096, 2], P(('ep', 'tp')), may hold values from 0.2 to 1
Outputs:
- mixed: bfloat16 [2048, 2048], P(('ep', 'tp'))
- moe_out: bfloat16 [4096, 2048], P(('ep', 'tp'))
The draws below stay inside these ranges and needn't reach their ends.
Inputs may be any that keep to these rules, and one draw needn't show every extreme that they name: `routes`: each row names 2 different experts. In each aligned block of 128 rows (the rows of one device) no expert is named by more than 48 rows, and in some block one expert is named by exactly 48 rows.
All inputs are finite; a program needn't handle non-finite values.
Results may differ from the reference program's by a relative error of at most 0.012.
Values may be sent and summed in bfloat16 or wider, within the bound.
A program may use at most 128 MiB of HBM per device.

```python
import math
import jax
import jax.numpy as jnp
import numpy as np
from jax import lax

D = 2048
HEADS = 8
KV_HEADS = 4
DH = 128
FF = 2048
TOP = 2
TOK_A = 256
TOK_B = 128
EXPERTS = 8
CAP = 48
GROUPS = 4
ATTENTION_TOKENS = 2048
TOKENS_B = 4096


def draw_key_bias(key, part):
    chooser = jax.random.uniform(jax.random.fold_in(key, 11), (HEADS,))
    slow_heads = chooser < 0.5
    slow_level = -jnp.log(ATTENTION_TOKENS * 23.0)
    levels = jnp.where(slow_heads, slow_level, -6.5)
    block_shift = jax.random.uniform(jax.random.fold_in(key, 12), (ATTENTION_TOKENS // TOK_A,), minval=-0.8, maxval=0.8)
    roughness = jax.random.uniform(jax.random.fold_in(key, 13), (ATTENTION_TOKENS, HEADS), minval=-1.0, maxval=1.0)
    release_point = jax.random.randint(jax.random.fold_in(key, 14), (3,), 0, ATTENTION_TOKENS)
    sequence_places = jnp.arange(ATTENTION_TOKENS)
    releasing_now = jnp.any(sequence_places[:, None] == release_point[None, :], axis=1)
    steady = levels[None, :] + jnp.repeat(block_shift, TOK_A)[:, None]
    drawn = jnp.where(releasing_now[:, None], -1.5, steady) + roughness
    return drawn.astype(jnp.float32).astype(jnp.bfloat16)


def shard_levels(rng, extent, split, smallest, largest):
    def one(dim, shards_of):
        draws = jax.random.uniform(jax.random.fold_in(jax.random.fold_in(rng, 6), dim), (shards_of,), jnp.float32, smallest / len(split), largest / len(split))
        return jnp.repeat(jnp.exp(draws), extent[dim] // shards_of).reshape((-1,) + (1,) * (len(extent) - dim - 1))

    factor_of = one(*split[0])
    for cut in split[1:]:
        factor_of = factor_of * one(*cut)
    return factor_of


def deal_out(stream_key, own, number, rows, number_of, top, limit, lean):
    ranking = jax.random.permutation(stream_key, number_of)
    crowded, ordinary = portions_of(number_of, rows * top, limit, lean, True), portions_of(number_of, rows * top, limit, lean, False)
    places = jnp.arange(number_of)

    def named(sizes, turn):
        used = int((sizes > 0).sum())
        fixed = max(1, used // 4)
        shifted = fixed + (places - fixed + turn * (used - fixed)) % max(1, number_of - fixed)
        return jnp.zeros((number_of,), jnp.int32).at[ranking[jnp.where(places < fixed, places, shifted)]].set(jnp.asarray(sizes, jnp.int32))

    sizes = jnp.where(number % 4 == 0, named(crowded, number // 4), named(ordinary, number - number // 4 - 1))
    mixed = jax.random.permutation(jax.random.fold_in(own, 3), number_of)
    donor, receiver = mixed[0:number_of // 2 * 2:2], mixed[1:number_of // 2 * 2:2]
    slack = jnp.minimum(sizes[donor] - 1, limit - sizes[receiver]) // 2
    slack = jnp.where((donor == ranking[0]) | (receiver == ranking[0]) | (sizes[receiver] == 0), 0, jnp.maximum(slack, 0))
    shifted = jax.random.randint(jax.random.fold_in(own, 4), (number_of // 2,), 0, 1 << 20) % (slack + 1)
    sizes = sizes.at[donor].add(-shifted).at[receiver].add(shifted)
    items = jnp.searchsorted(jnp.cumsum(sizes), jnp.arange(rows * top), side="right").astype(jnp.int32)
    table = items.reshape(top, rows).T
    table = table[jax.random.permutation(jax.random.fold_in(own, 1), rows)]
    turn = jax.random.randint(jax.random.fold_in(own, 2), (rows, 1), 0, top)
    return jnp.take_along_axis(table, (jnp.arange(top)[None, :] + turn) % top, axis=1)


def portions_of(count, total, most, skew, full):
    weights = [(1 << 20) // math.isqrt(standing ** skew) + 1 for standing in range(1, count + 1)]
    largest = most if full else min(most, max(-(-total // count), total * weights[0] // sum(weights)))
    least = 1 if total - largest >= count - 1 else 0
    given, spare = [largest] + [least] * (count - 1), total - largest - least * (count - 1)
    while spare > 0:
        candidates = [i for i in range(1, count) if given[i] < largest] or [i for i in range(1, count) if given[i] < most]
        mass, left = sum([weights[i] for i in candidates]), spare
        for i in candidates:
            more = min(most - given[i], max(1, left * weights[i] // mass), spare)
            given[i] = given[i] + more
            spare = spare - more
    return np.array(given)


def bell_draw(own_key, dims, width, bound, split=(), held_as=jnp.bfloat16):
    entries = width * jax.random.normal(own_key, dims, jnp.float32)
    if split:
        entries = entries * shard_levels(own_key, dims, split, -0.22, 0.18)
    return jnp.clip(entries, -bound, bound).astype(held_as)


def setup_inputs(seed: int = 0) -> dict:
    streams_of = jax.random.split(jax.random.key(seed), 13)
    queries = bell_draw(streams_of[0], (ATTENTION_TOKENS, HEADS, DH), 2.5, 15.0, ((0, 8), (1, 4)))
    keys = bell_draw(streams_of[1], (ATTENTION_TOKENS, KV_HEADS, DH), 1.0, 6.0, ((0, 8), (1, 4)))
    values = bell_draw(streams_of[2], (ATTENTION_TOKENS, KV_HEADS, DH), 1.0, 6.0, ((0, 8), (1, 4)))
    key_bias = draw_key_bias(jax.random.fold_in(streams_of[12], 71), 0)
    out_weight = bell_draw(streams_of[4], (HEADS * DH, D), (HEADS * DH) ** -0.5, 0.1875, ((0, 4),))
    tokens_b = bell_draw(streams_of[5], (TOKENS_B, D), 1.0, 6.0, ((0, 32),))
    moe_gain = jnp.clip(1.0 + 0.18 * jax.random.normal(streams_of[6], (D,), jnp.float32), 0.099609375, 1.8984375).astype(jnp.bfloat16)
    gate_weight = bell_draw(streams_of[7], (EXPERTS, D, FF), D ** -0.5, 0.125, ((0, 8), (2, 4)))
    up_weight = bell_draw(streams_of[8], (EXPERTS, D, FF), D ** -0.5, 0.125, ((0, 8), (2, 4)))
    down_weight = bell_draw(streams_of[9], (EXPERTS, FF, D), FF ** -0.5, 0.125, ((0, 8), (1, 4)))
    routes_keys = jax.random.split(jax.random.fold_in(streams_of[10], 1), TOKENS_B // TOK_B)
    routes_turns = jax.random.permutation(jax.random.fold_in(streams_of[10], 3), TOKENS_B // TOK_B)
    routes = jax.vmap(lambda own, number: deal_out(jax.random.fold_in(streams_of[10], 2), own, number, TOK_B, EXPERTS, TOP, CAP, 2))(routes_keys, routes_turns).reshape((TOKENS_B, TOP))
    route_weights = jnp.clip(0.2 + 0.8 * jax.random.uniform(streams_of[11], (TOKENS_B, TOP), jnp.float32) ** shard_levels(streams_of[11], (TOKENS_B, TOP), ((0, 32),), -0.2, 0.2), 0.2, 1.0)
    return dict(queries=queries, keys=keys, values=values, key_bias=key_bias, out_weight=out_weight, tokens_b=tokens_b, moe_gain=moe_gain, gate_weight=gate_weight, up_weight=up_weight, down_weight=down_weight, routes=routes, route_weights=route_weights)


def to_bf_and_back(partial_sum):
    return lax.optimization_barrier(partial_sum.astype(jnp.bfloat16)).astype(jnp.float32)

def stick_rows(query_block, first_pos, keys_all, values_all, bias_all):
    block_len = query_block.shape[0]
    group_size = HEADS // KV_HEADS
    query_f = query_block.astype(jnp.float32).reshape(block_len, KV_HEADS, group_size, DH)
    scores = jnp.einsum('rkgd,skd->kgrs', query_f, keys_all) / math.sqrt(DH)
    scores = scores + bias_all[:, :, None, :]
    query_pos = first_pos + jnp.arange(block_len, dtype=jnp.int32)
    key_pos = jnp.arange(ATTENTION_TOKENS, dtype=jnp.int32)
    earlier = key_pos[None, :] < query_pos[:, None]
    log_keep = jnp.where(earlier, jax.nn.log_sigmoid(-scores), 0.0)
    after = lax.cumsum(log_keep, axis=3, reverse=True) - log_keep
    weights = jnp.where(earlier, jnp.exp(jax.nn.log_sigmoid(scores) + after), 0.0).astype(jnp.bfloat16)
    attended = jnp.einsum('kgrs,skd->rkgd', weights.astype(jnp.float32), values_all)
    return attended.reshape(block_len, HEADS * DH).astype(jnp.bfloat16)

def reference(queries, keys, values, key_bias, out_weight, tokens_b, moe_gain, gate_weight, up_weight, down_weight, routes, route_weights):
    group_size = HEADS // KV_HEADS
    keys_all = keys.astype(jnp.float32)
    values_all = values.astype(jnp.float32)
    bias_all = jnp.transpose(key_bias.astype(jnp.float32).reshape(ATTENTION_TOKENS, KV_HEADS, group_size), (1, 2, 0))
    block_len = math.gcd(ATTENTION_TOKENS, 512)
    block_total = ATTENTION_TOKENS // block_len
    query_blocks = queries.reshape(block_total, block_len, HEADS, DH)
    first_positions = (jnp.arange(block_total) * block_len).astype(jnp.int32)

    def one_block(operands):
        return stick_rows(operands[0], operands[1], keys_all, values_all, bias_all)
    attended = lax.map(one_block, (query_blocks, first_positions)).reshape(ATTENTION_TOKENS, HEADS * DH)
    head_width = HEADS * DH // GROUPS
    mixed_sum = jnp.zeros((ATTENTION_TOKENS, D), jnp.float32)
    for group_no in range(GROUPS):
        lower = group_no * head_width
        partial_sum = jnp.dot(attended[:, lower:lower + head_width], out_weight[lower:lower + head_width], preferred_element_type=jnp.float32)
        mixed_sum = mixed_sum + to_bf_and_back(partial_sum)
    mixed = mixed_sum.astype(jnp.bfloat16)
    tokens_f = tokens_b.astype(jnp.float32)
    normed = (tokens_f * lax.rsqrt(lax.optimization_barrier(jnp.mean(tokens_f * tokens_f, axis=1, keepdims=True)) + 1e-06) * moe_gain.astype(jnp.float32)).astype(jnp.bfloat16)
    block_count = TOKENS_B // TOK_B
    flattened_expert_list = routes.reshape(block_count, TOK_B * TOP)
    onehot = (flattened_expert_list[:, :, None] == jnp.arange(EXPERTS, dtype=jnp.int32)[None, None, :]).astype(jnp.int32)
    earlier_count = jnp.cumsum(onehot, axis=1) - onehot
    slot_index = lax.optimization_barrier(jnp.sum(earlier_count * onehot, axis=2))
    block_ids = jnp.arange(block_count, dtype=jnp.int32)[:, None]
    place = (block_ids * CAP + slot_index).astype(jnp.int32)
    token_ids = (block_ids * TOK_B + jnp.arange(TOK_B * TOP, dtype=jnp.int32)[None, :] // TOP).astype(jnp.int32)
    table_token = jnp.zeros((EXPERTS, block_count * CAP), jnp.int32).at[flattened_expert_list.reshape(-1), place.reshape(-1)].set(token_ids.reshape(-1))
    table_weight = jnp.zeros((EXPERTS, block_count * CAP), jnp.float32).at[flattened_expert_list.reshape(-1), place.reshape(-1)].set(route_weights.astype(jnp.float32).reshape(-1))
    unit_width = FF // GROUPS

    def one_expert(carry, operands):
        gate_e, up_e, down_e, token_list, weight_list = operands
        picked = jnp.take(normed, token_list, axis=0)
        gate_val = jnp.dot(picked, gate_e, preferred_element_type=jnp.float32)
        up_val = jnp.dot(picked, up_e, preferred_element_type=jnp.float32)
        hidden = (jax.nn.silu(gate_val) * up_val).astype(jnp.bfloat16)
        expert_sum = jnp.zeros((token_list.shape[0], D), jnp.float32)
        for group_no in range(GROUPS):
            lower = group_no * unit_width
            partial_sum = jnp.dot(hidden[:, lower:lower + unit_width], down_e[lower:lower + unit_width], preferred_element_type=jnp.float32)
            expert_sum = expert_sum + to_bf_and_back(partial_sum)
        result = to_bf_and_back(expert_sum)
        carry = carry.at[token_list].add(weight_list[:, None] * result)
        return (carry, None)
    moe_total = lax.scan(one_expert, jnp.zeros((TOKENS_B, D), jnp.float32), (gate_weight, up_weight, down_weight, table_token, table_weight))[0]
    moe_out = moe_total.astype(jnp.bfloat16)
    return (mixed, moe_out)
```

```python
import functools
import math

import jax
import jax.numpy as jnp
from jax import lax
from jax.experimental import pallas as pl
from jax.experimental.pallas import tpu as pltpu
from jax.sharding import PartitionSpec as P

MESH = pl.DeviceIdType.MESH
F32, BF16 = jnp.float32, jnp.bfloat16

SLOTS = 34
SENDS = ((5, 1, 4, 3, 6, 2, 7), (4, 3, 7, 2, 1, 5, 6))
PLAN = {
    'part': ((0, 5505024, 16805888, 2622976, 3), (0, 1441792, 262149, 7350272, 768)),
    'fin': ((0, 0, 72351744, 6320128, 12584), (0, 0, 1536, 336, 3612744)),
    'dot': ((0, 33574977, 526080, 12294, 0), (0, 266326, 131120, 28680, 0)),
    'relay': ((55706640, 526080, 96, 0, 0), (271713, 2096, 28672, 0, 0)),
    'both': ((4198400, 2293840, 100665351, 0, 0), (90177536, 50463760, 134217728, 112, 0)),
    'kvf': ((1, 33554432, 0, 262192, 0), (65536, 0, 770, 4, 0)),
    'att': ((256, 0, 204800, 141952260, 0), (0, 1048576, 4390944, 141971456, 0)),
    'mix1': ((0, 0, 0, 0, 1), (0, 0, 0, 0, 256)),
    'mix2': ((0, 0, 0, 0, 1), (0, 0, 0, 0, 256)),
}


def remote(src, dst, send_sem, recv_sem, **where):
    return pltpu.make_async_remote_copy(
        src_ref=src, dst_ref=dst, send_sem=send_sem, recv_sem=recv_sem,
        device_id=where, device_id_type=MESH,
    )


def dot(a, b):
    return jnp.dot(a, b, preferred_element_type=F32)


def flip(a, b, n):
    out, bit = 0, 1
    while bit < n:
        p, q = (a // bit) % 2, (b // bit) % 2
        out = out + bit * (p + q - 2 * p * q)
        bit *= 2
    return out


def columns(rows_ref):
    values = rows_ref[...].astype(F32)
    top, tok = values.shape
    return [
        jnp.transpose(jnp.broadcast_to(values[c : c + 1, :], (128, tok)))[:, 0:1] for c in range(top)
    ]


def slots_of(routes, me, ep, cap):
    tok, top = routes[0].shape[0], len(routes)
    lanes = max(128, -(-ep // 128) * 128)
    lane = lax.broadcasted_iota(jnp.int32, (tok, lanes), 1)
    picks = [(lane == routes[c]).astype(F32) for c in range(top)]
    named = functools.reduce(lambda a, b: a + b, picks)
    row = lax.broadcasted_iota(jnp.int32, (tok, tok), 0)
    col = lax.broadcasted_iota(jnp.int32, (tok, tok), 1)
    earlier = dot((col < row).astype(F32).astype(BF16), named.astype(BF16))
    places = []
    for c in range(top):
        slot = jnp.sum(earlier * picks[c], axis=1, keepdims=True).astype(jnp.int32)
        places.append((routes[c] ^ me) * cap + slot)
    return places


def moe_kernel(
    ep, tp_n, cap, heads,
    routes_ref, weights_ref, tokens_ref, gain_ref, q_ref, keys_ref, values_ref, bias_ref, wo_ref,
    gate_hbm, up_hbm, down_hbm, mixed_ref, out_ref,
    gate, up, down, outbound, rows, core_in, x_in, ret,
    kv, kb, acc, carried, part, mix_core, mix_x,
    w_sem, a_s, a_r, bx_s, bx_r, bc_s, bc_r, bd_s, bd_r,
    p0_s, p0_r, p1_s, p1_r, q_s, q_r, r_s, r_r,
    c_s, cb_s, m_s, mb_s, kv_r, kb_r,
    m0_s, m0_r, m1_s, m1_r, mq_s, mq_r,
):
    me, tp = lax.axis_index("ep"), lax.axis_index("tp")
    mate = tp + 1 - 2 * (tp % 2)
    across = (tp + 2) % 4
    mate_across = (mate + 2) % 4
    beside = me + 1 - 2 * (me % 2)
    place = ((me // 2 + 1) // 2) % 2
    span, dim = keys_ref.shape
    tok, width = tokens_ref.shape

    loads = [
        pltpu.make_async_copy(src.at[0], dst, w_sem.at[n])
        for n, (src, dst) in enumerate(((gate_hbm, gate), (up_hbm, up), (down_hbm, down)))
    ]
    for load in loads:
        load.start()

    barrier = pltpu.get_barrier_semaphore()

    def greet(k, _):
        pl.semaphore_signal(barrier, inc=1, device_id={"ep": (me + k) % ep}, device_id_type=MESH)
        return 0

    lax.fori_loop(1, ep, greet, 0)
    for other in (mate, across):
        pl.semaphore_signal(barrier, inc=1, device_id={"tp": other}, device_id_type=MESH)

    kv[me, 0:span] = keys_ref[...]
    kv[me, span : 2 * span] = values_ref[...]
    kb[me] = bias_ref[...]
    acc[...] = jnp.zeros_like(acc)
    carried[...] = jnp.zeros_like(carried)

    places = slots_of([c.astype(jnp.int32) for c in columns(routes_ref)], me, ep, cap)
    slot_id = lax.broadcasted_iota(jnp.int32, (tok, ep * cap), 1)
    hits = [(slot_id == place).astype(F32) for place in places]
    chosen = functools.reduce(lambda a, b: a + b, hits)
    tokens = tokens_ref[...].astype(F32)
    mean = jnp.mean(tokens * tokens, axis=1, keepdims=True)
    normed = (tokens * lax.rsqrt(mean + 1e-06) * gain_ref[...].astype(F32)).astype(BF16)
    packed = dot(jnp.transpose(chosen).astype(BF16), normed).astype(BF16)
    outbound[...] = packed.reshape(ep, cap, width)
    rows[0, tp] = packed[:cap]

    pl.semaphore_wait(barrier, ep + 1)

    planned = ep == 8

    def pick(choices, n):
        value = choices[-1]
        for c in range(len(choices) - 1):
            value = jnp.where(n == c, choices[c], value)
        return value

    def plan(i):
        if planned:
            word, digit = i // 7, 4 * (i % 7)
            work = {}
            for stage, table in PLAN.items():
                packed = pick([pick(row, place) for row in zip(*table)], word)
                entry = (packed >> digit) & 15
                work[stage] = (entry > 0, entry - 1)
            return work

        def lagged(lag):
            return (i >= lag) & (i < ep + lag), i - lag

        def turned(lag):
            active, p = lagged(lag)
            return active, jnp.where(p < ep - 2, p + 2, ep - 1 - p)

        return {
            "part": turned(5), "fin": turned(6), "dot": lagged(2), "relay": lagged(0),
            "both": lagged(1), "kvf": ((i == 0) | (i % 2 == 1), (i + 1) // 2), "att": lagged(2),
            "mix1": (i == ep + 2, 0), "mix2": (i == ep + 3, 0),
        }

    def dispatch(k):
        return remote(outbound.at[k], rows.at[k, tp], a_s.at[k], a_r.at[k], ep=flip(me, k, ep))

    def relay_across(k):
        return remote(rows.at[k, tp], rows.at[k, tp], bx_s.at[k], bx_r.at[k], tp=across)

    def relay_mate(k):
        return remote(rows.at[k, tp], rows.at[k, tp], bc_s.at[k], bc_r.at[k], tp=mate)

    def relay_both(k):
        return remote(rows.at[k, across], rows.at[k, across], bd_s.at[k], bd_r.at[k], tp=mate)

    def part_mate(k):
        return remote(rows.at[k, mate], core_in.at[k, 0], p0_s.at[k], p0_r.at[k], tp=mate)

    def part_mate_across(k):
        return remote(rows.at[k, mate_across], core_in.at[k, 1], p1_s.at[k], p1_r.at[k], tp=mate)

    def part_across(k):
        return remote(core_in.at[k, 1], x_in.at[k], q_s.at[k], q_r.at[k], tp=across)

    def give_back(k):
        return remote(x_in.at[k], ret.at[k], r_s.at[k], r_r.at[k], ep=flip(me, k, ep))

    def along(s):
        return (
            remote(kv.at[s], kv.at[s], c_s.at[s], kv_r.at[s], ep=(me + 2) % ep),
            remote(kb.at[s], kb.at[s], cb_s.at[s], kb_r.at[s], ep=(me + 2) % ep),
        )

    def aside(s):
        return (
            remote(kv.at[s], kv.at[s], m_s.at[s], kv_r.at[s], ep=beside),
            remote(kb.at[s], kb.at[s], mb_s.at[s], kb_r.at[s], ep=beside),
        )

    def pass_keys(j, act):
        s = me - 2 * j

        @pl.when((s >= 0) & (me + 2 < ep))
        def _():
            for copy in along(s):
                act(copy)

        @pl.when((s >= 0) & ((me % 2 == 0) | (j > 0)))
        def _():
            for copy in aside(s):
                act(copy)

    if planned:
        for turn in zip(*SENDS):
            dispatch(pick(turn, place)).start()
    else:
        def send(k, _):
            dispatch(k).start()
            return 0

        lax.fori_loop(1, ep, send, 0)

    mix_far = remote(part.at[mate_across], mix_core.at[1], m1_s, m1_r, tp=mate)
    mix_near = remote(part.at[mate], mix_core.at[0], m0_s, m0_r, tp=mate)
    mix_over = remote(mix_core.at[1], mix_x, mq_s, mq_r, tp=across)

    total_rows = heads * span
    nt = (((1,), (1,)), ((), ()))

    def attend(n):
        s = me - n
        key_no = lax.broadcasted_iota(jnp.int32, (total_rows, span), 1)
        query_no = lax.broadcasted_iota(jnp.int32, (total_rows, span), 0) % span
        tri = (
            lax.broadcasted_iota(jnp.int32, (span, span), 0)
            > lax.broadcasted_iota(jnp.int32, (span, span), 1)
        ).astype(F32).astype(BF16)
        bias = kb[s].astype(F32)
        scores = lax.dot_general(q_ref[...], kv[s, 0:span], nt, preferred_element_type=F32)
        scores = scores * (1.0 / math.sqrt(dim)) + jnp.concatenate(
            [jnp.broadcast_to(bias[h : h + 1, :], (span, span)) for h in range(heads)], axis=0
        )
        seen = (key_no < query_no) | (n > 0)
        soft = jnp.log(1.0 + jnp.exp(-jnp.abs(scores)))
        log_take = jnp.minimum(scores, 0.0) - soft
        log_keep = jnp.where(seen, log_take - scores, 0.0)
        high = log_keep.astype(BF16)
        low = (log_keep - high.astype(F32)).astype(BF16)
        after = dot(high, tri) + dot(low, tri)
        before = carried[:, 0:1]
        stick = jnp.where(seen, jnp.exp(log_take + after + before), 0.0).astype(BF16)
        acc[...] += dot(stick, kv[s, span : 2 * span])
        carried[...] = jnp.broadcast_to(
            before + jnp.sum(log_keep, axis=1, keepdims=True), carried.shape
        )

    def project():
        mixed = functools.reduce(
            lambda a, b: a + b,
            [
                dot(acc[h * span : (h + 1) * span].astype(BF16), wo_ref[h * dim : (h + 1) * dim, :])
                for h in range(heads)
            ],
        )
        part[...] = mixed.astype(BF16).reshape(part.shape)

    def step(i, _):
        work = plan(i)

        @pl.when(work["part"][0])
        def _():
            k = work["part"][1]
            part_mate(k).wait()
            part_mate_across(k).wait()
            core_in[k, 1] = (core_in[k, 1].astype(F32) + rows[k, across].astype(F32)).astype(BF16)
            part_across(k).start()

        @pl.when(work["fin"][0])
        def _():
            k = work["fin"][1]
            part_across(k).wait()
            total = (
                rows[k, tp].astype(F32) + core_in[k, 0].astype(F32) + x_in[k].astype(F32)
            ).astype(BF16)

            @pl.when(k > 0)
            def _():
                x_in[k] = total
                give_back(k).start()

            @pl.when(k == 0)
            def _():
                ret[0] = total

        @pl.when(work["dot"][0])
        def _():
            k = work["dot"][1]
            relay_mate(k).wait()
            relay_both(k).wait()
            relay_across(k).wait_send()
            x = rows[k].reshape(tp_n * cap, width)
            gated = dot(x, gate[...])
            lifted = dot(x, up[...])
            hidden = (gated / (1.0 + jnp.exp(-gated)) * lifted).astype(BF16)
            rows[k] = dot(hidden, down[...]).astype(BF16).reshape(tp_n, cap, width)
            part_mate(k).start()
            part_mate_across(k).start()

        @pl.when(work["relay"][0])
        def _():
            k = work["relay"][1]

            @pl.when(k > 0)
            def _():
                dispatch(k).wait_recv()

            relay_across(k).start()
            relay_mate(k).start()

        @pl.when(work["both"][0])
        def _():
            k = work["both"][1]
            relay_across(k).wait_recv()
            relay_both(k).start()

        @pl.when(work["kvf"][0] & (me - 2 * work["kvf"][1] >= 0))
        def _():
            j = work["kvf"][1]

            @pl.when(j > 0)
            def _():
                for copy in along(me - 2 * j):
                    copy.wait_recv()

            pass_keys(j, lambda copy: copy.start())

        @pl.when(work["att"][0] & (work["att"][1] <= me))
        def _():
            n = work["att"][1]

            @pl.when(n % 2 == 1)
            def _():
                for copy in aside(me - n):
                    copy.wait_recv()

            attend(n)

        @pl.when(work["mix1"][0])
        def _():
            project()
            mix_far.start()
            mix_near.start()

        @pl.when(work["mix2"][0])
        def _():
            mix_far.wait()
            mix_core[1] = (mix_core[1].astype(F32) + part[across].astype(F32)).astype(BF16)
            mix_over.start()

        return 0

    for load in loads:
        load.wait()
    lax.fori_loop(0, SLOTS if planned else ep + 6, step, 0)

    def drain(j, _):
        pass_keys(j, lambda copy: copy.wait_send())
        return 0

    lax.fori_loop(0, ep // 2, drain, 0)
    mix_near.wait()
    mix_over.wait()
    mixed_ref[...] = (
        part[tp].astype(F32) + mix_core[0].astype(F32) + mix_x[...].astype(F32)
    ).astype(BF16)

    def finish(k, _):
        dispatch(k).wait_send()
        give_back(k).wait()
        return 0

    lax.fori_loop(1, ep, finish, 0)
    weights = columns(weights_ref)
    mix = functools.reduce(
        lambda a, b: a + b, [hit * weights[c] for c, hit in enumerate(hits)]
    )
    high = mix.astype(BF16)
    low = (mix - high.astype(F32)).astype(BF16)
    results = ret[...].reshape(ep * cap, width)
    out_ref[...] = (dot(high, results) + dot(low, results)).astype(BF16)


def body(
    queries, keys, values, key_bias, out_weight, tokens_b, moe_gain,
    gate_weight, up_weight, down_weight, routes, route_weights,
):
    ep, tp_n = lax.axis_size("ep"), lax.axis_size("tp")
    tok, width = tokens_b.shape
    top = routes.shape[1]
    units = gate_weight.shape[2]
    experts = ep * gate_weight.shape[0]
    capacity = max(2, 3 * top * tok // (2 * experts))
    cap = -(-capacity // 16) * 16
    span, heads, dim = queries.shape
    share = span // tp_n
    vmem = pl.BlockSpec(memory_space=pltpu.VMEM)
    hbm = pl.BlockSpec(memory_space=pl.ANY)
    dma = pltpu.SemaphoreType.DMA
    return pl.pallas_call(
        functools.partial(moe_kernel, ep, tp_n, cap, heads),
        out_shape=(
            jax.ShapeDtypeStruct((share, width), BF16),
            jax.ShapeDtypeStruct((tok, width), BF16),
        ),
        in_specs=[vmem] * 9 + [hbm] * 3,
        out_specs=(vmem, vmem),
        scratch_shapes=[
            pltpu.VMEM((width, units), BF16),
            pltpu.VMEM((width, units), BF16),
            pltpu.VMEM((units, width), BF16),
            pltpu.VMEM((ep, cap, width), BF16),
            pltpu.VMEM((ep, tp_n, cap, width), BF16),
            pltpu.VMEM((ep, 2, cap, width), BF16),
            pltpu.VMEM((ep, cap, width), BF16),
            pltpu.VMEM((ep, cap, width), BF16),
            pltpu.VMEM((ep, 2 * span, dim), BF16),
            pltpu.VMEM((ep, heads, span), BF16),
            pltpu.VMEM((heads * span, dim), F32),
            pltpu.VMEM((heads * span, 128), F32),
            pltpu.VMEM((tp_n, share, width), BF16),
            pltpu.VMEM((2, share, width), BF16),
            pltpu.VMEM((share, width), BF16),
            dma((3,)),
        ] + [dma((ep,))] * 22 + [dma] * 6,
        compiler_params=pltpu.CompilerParams(
            collective_id=0, has_side_effects=True, vmem_limit_bytes=67043328
        ),
        cost_estimate=pl.CostEstimate(
            flops=6 * ep * tp_n * cap * width * units, bytes_accessed=6 * width * units,
            transcendentals=0,
        ),
        name="layer",
    )(
        jnp.transpose(routes), jnp.transpose(route_weights), tokens_b, moe_gain.reshape(1, width),
        jnp.transpose(queries, (1, 0, 2)).reshape(heads * span, dim),
        keys[:, 0], values[:, 0], jnp.transpose(key_bias), out_weight,
        gate_weight, up_weight, down_weight,
    )


def solution(mesh):
    in_specs = (
        P("ep", "tp", None),
        P("ep", "tp", None),
        P("ep", "tp", None),
        P("ep", "tp"),
        P("tp", None),
        P(("ep", "tp"), None),
        P(),
        P("ep", None, "tp"),
        P("ep", None, "tp"),
        P("ep", "tp", None),
        P(("ep", "tp"), None),
        P(("ep", "tp"), None),
    )
    out_specs = (P(("ep", "tp"), None), P(("ep", "tp"), None))
    return jax.shard_map(body, mesh=mesh, in_specs=in_specs, out_specs=out_specs, check_vma=False)
```

```python
import functools
import math

import jax
import jax.numpy as jnp
from jax import lax
from jax.experimental import pallas as pl
from jax.experimental.pallas import tpu as pltpu
from jax.sharding import PartitionSpec as P

MESH = pl.DeviceIdType.MESH
F32, BF16 = jnp.float32, jnp.bfloat16

SLOTS = 34
SENDS = ((6, 4, 3, 2, 1, 5, 7), (1, 5, 6, 7, 2, 3, 4))
PLAN = {
    'part': ((0, 100663298, 138413824, 1246464, 0), (0, 6619136, 262256, 3146368, 4096)),
    'fin': ((0, 0, 24576, 42205296, 4869), (0, 0, 100663301, 67108976, 1245824)),
    'dot': ((131072, 4587536, 2055, 12293, 0), (0, 117834757, 8519680, 77824, 0)),
    'relay': ((73414433, 128, 80, 0, 0), (57099553, 524288, 0, 0, 0)),
    'both': ((66048, 29510, 327808, 0, 0), (20480, 30272, 98816, 768, 0)),
    'kvf': ((0, 256, 50331650, 1024, 0), (16, 2097152, 262192, 0, 0)),
    'att': ((0, 16777216, 8192, 105923328, 135), (0, 1, 33554432, 105907203, 32775)),
    'mix1': ((0, 0, 0, 0, 16), (0, 0, 0, 0, 4096)),
    'mix2': ((0, 0, 0, 0, 16), (0, 0, 0, 0, 65536)),
}


def remote(src, dst, send_sem, recv_sem, **where):
    return pltpu.make_async_remote_copy(
        src_ref=src, dst_ref=dst, send_sem=send_sem, recv_sem=recv_sem,
        device_id=where, device_id_type=MESH,
    )


def dot(a, b):
    return jnp.dot(a, b, preferred_element_type=F32)


def flip(a, b, n):
    out, bit = 0, 1
    while bit < n:
        p, q = (a // bit) % 2, (b // bit) % 2
        out = out + bit * (p + q - 2 * p * q)
        bit *= 2
    return out


def columns(rows_ref):
    values = rows_ref[...].astype(F32)
    top, tok = values.shape
    return [
        jnp.transpose(jnp.broadcast_to(values[c : c + 1, :], (128, tok)))[:, 0:1] for c in range(top)
    ]


def slots_of(routes, me, ep, cap):
    tok, top = routes[0].shape[0], len(routes)
    lanes = max(128, -(-ep // 128) * 128)
    lane = lax.broadcasted_iota(jnp.int32, (tok, lanes), 1)
    picks = [(lane == routes[c]).astype(F32) for c in range(top)]
    named = functools.reduce(lambda a, b: a + b, picks)
    row = lax.broadcasted_iota(jnp.int32, (tok, tok), 0)
    col = lax.broadcasted_iota(jnp.int32, (tok, tok), 1)
    earlier = dot((col < row).astype(F32).astype(BF16), named.astype(BF16))
    places = []
    for c in range(top):
        slot = jnp.sum(earlier * picks[c], axis=1, keepdims=True).astype(jnp.int32)
        places.append((routes[c] ^ me) * cap + slot)
    return places


def moe_kernel(
    ep, tp_n, cap, heads,
    routes_ref, weights_ref, tokens_ref, gain_ref, q_ref, keys_ref, values_ref, bias_ref, wo_ref,
    gate_hbm, up_hbm, down_hbm, mixed_ref, out_ref,
    gate, up, down, outbound, rows, core_in, x_in, ret,
    qs, kv, kb, acc, carried, part, mix_core, mix_x,
    w_sem, a_s, a_r, bx_s, bx_r, bc_s, bc_r, bd_s, bd_r,
    p0_s, p0_r, p1_s, p1_r, q_s, q_r, r_s, r_r,
    c_s, cb_s, m_s, mb_s, kv_r, kb_r,
    m0_s, m0_r, m1_s, m1_r, mq_s, mq_r,
):
    me, tp = lax.axis_index("ep"), lax.axis_index("tp")
    mate = tp + 1 - 2 * (tp % 2)
    across = (tp + 2) % 4
    mate_across = (mate + 2) % 4
    beside = me + 1 - 2 * (me % 2)
    place = ((me // 2 + 1) // 2) % 2
    span, dim = keys_ref.shape
    tok, width = tokens_ref.shape

    loads = [
        pltpu.make_async_copy(src.at[0], dst, w_sem.at[n])
        for n, (src, dst) in enumerate(((gate_hbm, gate), (up_hbm, up), (down_hbm, down)))
    ]
    for load in loads:
        load.start()

    barrier = pltpu.get_barrier_semaphore()

    def greet(k, _):
        pl.semaphore_signal(barrier, inc=1, device_id={"ep": (me + k) % ep}, device_id_type=MESH)
        return 0

    lax.fori_loop(1, ep, greet, 0)
    for other in (mate, across):
        pl.semaphore_signal(barrier, inc=1, device_id={"tp": other}, device_id_type=MESH)

    kv[me, 0:span] = keys_ref[...]
    kv[me, span : 2 * span] = values_ref[...]
    kb[me] = bias_ref[...]
    wide = q_ref[...].astype(F32)
    for h in range(heads):
        qs[h * span : (h + 1) * span] = wide[:, h, :].astype(BF16)
    acc[...] = jnp.zeros_like(acc)
    carried[...] = jnp.zeros_like(carried)

    places = slots_of([c.astype(jnp.int32) for c in columns(routes_ref)], me, ep, cap)
    slot_id = lax.broadcasted_iota(jnp.int32, (tok, ep * cap), 1)
    hits = [(slot_id == place).astype(F32) for place in places]
    chosen = functools.reduce(lambda a, b: a + b, hits)
    tokens = tokens_ref[...].astype(F32)
    mean = jnp.mean(tokens * tokens, axis=1, keepdims=True)
    normed = (tokens * lax.rsqrt(mean + 1e-06) * gain_ref[...].astype(F32).reshape(1, width)).astype(BF16)
    packed = dot(jnp.transpose(chosen).astype(BF16), normed).astype(BF16)
    outbound[...] = packed.reshape(ep, cap, width)
    rows[0, tp] = packed[:cap]

    pl.semaphore_wait(barrier, ep + 1)

    planned = ep == 8

    def pick(choices, n):
        value = choices[-1]
        for c in range(len(choices) - 1):
            value = jnp.where(n == c, choices[c], value)
        return value

    def plan(i):
        if planned:
            word, digit = i // 7, 4 * (i % 7)
            work = {}
            for stage, table in PLAN.items():
                packed = pick([pick(row, place) for row in zip(*table)], word)
                entry = (packed >> digit) & 15
                work[stage] = (entry > 0, entry - 1)
            return work

        def lagged(lag):
            return (i >= lag) & (i < ep + lag), i - lag

        def turned(lag):
            active, p = lagged(lag)
            return active, jnp.where(p < ep - 2, p + 2, ep - 1 - p)

        return {
            "part": turned(5), "fin": turned(6), "dot": lagged(2), "relay": lagged(0),
            "both": lagged(1), "kvf": ((i == 0) | (i % 2 == 1), (i + 1) // 2), "att": lagged(2),
            "mix1": (i == ep + 2, 0), "mix2": (i == ep + 3, 0),
        }

    def dispatch(k):
        return remote(outbound.at[k], rows.at[k, tp], a_s.at[k], a_r.at[k], ep=flip(me, k, ep))

    def relay_across(k):
        return remote(rows.at[k, tp], rows.at[k, tp], bx_s.at[k], bx_r.at[k], tp=across)

    def relay_mate(k):
        return remote(rows.at[k, tp], rows.at[k, tp], bc_s.at[k], bc_r.at[k], tp=mate)

    def relay_both(k):
        return remote(rows.at[k, across], rows.at[k, across], bd_s.at[k], bd_r.at[k], tp=mate)

    def part_mate(k):
        return remote(rows.at[k, mate], core_in.at[k, 0], p0_s.at[k], p0_r.at[k], tp=mate)

    def part_mate_across(k):
        return remote(rows.at[k, mate_across], core_in.at[k, 1], p1_s.at[k], p1_r.at[k], tp=mate)

    def part_across(k):
        return remote(core_in.at[k, 1], x_in.at[k], q_s.at[k], q_r.at[k], tp=across)

    def give_back(k):
        return remote(x_in.at[k], ret.at[k], r_s.at[k], r_r.at[k], ep=flip(me, k, ep))

    def along(s):
        return (
            remote(kv.at[s], kv.at[s], c_s.at[s], kv_r.at[s], ep=(me + 2) % ep),
            remote(kb.at[s], kb.at[s], cb_s.at[s], kb_r.at[s], ep=(me + 2) % ep),
        )

    def aside(s):
        return (
            remote(kv.at[s], kv.at[s], m_s.at[s], kv_r.at[s], ep=beside),
            remote(kb.at[s], kb.at[s], mb_s.at[s], kb_r.at[s], ep=beside),
        )

    def pass_keys(j, act):
        s = me - 2 * j

        @pl.when((s >= 0) & (me + 2 < ep))
        def _():
            for copy in along(s):
                act(copy)

        @pl.when((s >= 0) & ((me % 2 == 0) | (j > 0)))
        def _():
            for copy in aside(s):
                act(copy)

    if planned:
        for turn in zip(*SENDS):
            dispatch(pick(turn, place)).start()
    else:
        def send(k, _):
            dispatch(k).start()
            return 0

        lax.fori_loop(1, ep, send, 0)

    mix_far = remote(part.at[mate_across], mix_core.at[1], m1_s, m1_r, tp=mate)
    mix_near = remote(part.at[mate], mix_core.at[0], m0_s, m0_r, tp=mate)
    mix_over = remote(mix_core.at[1], mix_x, mq_s, mq_r, tp=across)

    total_rows = heads * span
    nt = (((1,), (1,)), ((), ()))

    def attend(n):
        s = me - n
        key_no = lax.broadcasted_iota(jnp.int32, (total_rows, span), 1)
        query_no = lax.broadcasted_iota(jnp.int32, (total_rows, span), 0) % span
        tri = (
            lax.broadcasted_iota(jnp.int32, (span, span), 0)
            > lax.broadcasted_iota(jnp.int32, (span, span), 1)
        ).astype(F32).astype(BF16)
        bias = kb[s].astype(F32)
        scores = lax.dot_general(qs[...], kv[s, 0:span], nt, preferred_element_type=F32)
        scores = scores * (1.0 / math.sqrt(dim)) + jnp.concatenate(
            [jnp.broadcast_to(bias[h : h + 1, :], (span, span)) for h in range(heads)], axis=0
        )
        seen = (key_no < query_no) | (n > 0)
        soft = jnp.log(1.0 + jnp.exp(-jnp.abs(scores)))
        log_take = jnp.minimum(scores, 0.0) - soft
        log_keep = jnp.where(seen, log_take - scores, 0.0)
        high = log_keep.astype(BF16)
        low = (log_keep - high.astype(F32)).astype(BF16)
        after = dot(high, tri) + dot(low, tri)
        before = carried[:, 0:1]
        stick = jnp.where(seen, jnp.exp(log_take + after + before), 0.0).astype(BF16)
        acc[...] += dot(stick, kv[s, span : 2 * span])
        carried[...] = jnp.broadcast_to(
            before + jnp.sum(log_keep, axis=1, keepdims=True), carried.shape
        )

    def project():
        mixed = functools.reduce(
            lambda a, b: a + b,
            [
                dot(acc[h * span : (h + 1) * span].astype(BF16), wo_ref[h * dim : (h + 1) * dim, :])
                for h in range(heads)
            ],
        )
        part[...] = mixed.astype(BF16).reshape(part.shape)

    def step(i, _):
        work = plan(i)

        @pl.when(work["part"][0])
        def _():
            k = work["part"][1]
            part_mate(k).wait()
            part_mate_across(k).wait()
            core_in[k, 1] = (core_in[k, 1].astype(F32) + rows[k, across].astype(F32)).astype(BF16)
            part_across(k).start()

        @pl.when(work["fin"][0])
        def _():
            k = work["fin"][1]
            part_across(k).wait()
            total = (
                rows[k, tp].astype(F32) + core_in[k, 0].astype(F32) + x_in[k].astype(F32)
            ).astype(BF16)

            @pl.when(k > 0)
            def _():
                x_in[k] = total
                give_back(k).start()

            @pl.when(k == 0)
            def _():
                ret[0] = total

        @pl.when(work["dot"][0])
        def _():
            k = work["dot"][1]
            relay_mate(k).wait()
            relay_both(k).wait()
            relay_across(k).wait_send()
            x = rows[k].reshape(tp_n * cap, width)
            gated = dot(x, gate[...])
            lifted = dot(x, up[...])
            hidden = (gated / (1.0 + jnp.exp(-gated)) * lifted).astype(BF16)
            rows[k] = dot(hidden, down[...]).astype(BF16).reshape(tp_n, cap, width)
            part_mate(k).start()
            part_mate_across(k).start()

        @pl.when(work["relay"][0])
        def _():
            k = work["relay"][1]

            @pl.when(k > 0)
            def _():
                dispatch(k).wait_recv()

            relay_across(k).start()
            relay_mate(k).start()

        @pl.when(work["both"][0])
        def _():
            k = work["both"][1]
            relay_across(k).wait_recv()
            relay_both(k).start()

        @pl.when(work["kvf"][0] & (me - 2 * work["kvf"][1] >= 0))
        def _():
            j = work["kvf"][1]

            @pl.when(j > 0)
            def _():
                for copy in along(me - 2 * j):
                    copy.wait_recv()

            pass_keys(j, lambda copy: copy.start())

        @pl.when(work["att"][0] & (work["att"][1] <= me))
        def _():
            n = work["att"][1]

            @pl.when(n % 2 == 1)
            def _():
                for copy in aside(me - n):
                    copy.wait_recv()

            attend(n)

        @pl.when(work["mix1"][0])
        def _():
            project()
            mix_far.start()
            mix_near.start()

        @pl.when(work["mix2"][0])
        def _():
            mix_far.wait()
            mix_core[1] = (mix_core[1].astype(F32) + part[across].astype(F32)).astype(BF16)
            mix_over.start()

        return 0

    for load in loads:
        load.wait()
    lax.fori_loop(0, SLOTS if planned else ep + 6, step, 0)

    def drain(j, _):
        pass_keys(j, lambda copy: copy.wait_send())
        return 0

    lax.fori_loop(0, ep // 2, drain, 0)
    mix_near.wait()
    mix_over.wait()
    mixed_ref[...] = (
        part[tp].astype(F32) + mix_core[0].astype(F32) + mix_x[...].astype(F32)
    ).astype(BF16)

    def finish(k, _):
        dispatch(k).wait_send()
        give_back(k).wait()
        return 0

    lax.fori_loop(1, ep, finish, 0)
    weights = columns(weights_ref)
    mix = functools.reduce(
        lambda a, b: a + b, [hit * weights[c] for c, hit in enumerate(hits)]
    )
    high = mix.astype(BF16)
    low = (mix - high.astype(F32)).astype(BF16)
    results = ret[...].reshape(ep * cap, width)
    out_ref[...] = (dot(high, results) + dot(low, results)).astype(BF16)


def body(
    queries, keys, values, key_bias, out_weight, tokens_b, moe_gain,
    gate_weight, up_weight, down_weight, routes, route_weights,
):
    ep, tp_n = lax.axis_size("ep"), lax.axis_size("tp")
    tok, width = tokens_b.shape
    top = routes.shape[1]
    units = gate_weight.shape[2]
    experts = ep * gate_weight.shape[0]
    capacity = max(2, 3 * top * tok // (2 * experts))
    cap = -(-capacity // 16) * 16
    span, heads, dim = queries.shape
    share = span // tp_n
    vmem = pl.BlockSpec(memory_space=pltpu.VMEM)
    hbm = pl.BlockSpec(memory_space=pl.ANY)
    dma = pltpu.SemaphoreType.DMA
    return pl.pallas_call(
        functools.partial(moe_kernel, ep, tp_n, cap, heads),
        out_shape=(
            jax.ShapeDtypeStruct((share, width), BF16),
            jax.ShapeDtypeStruct((tok, width), BF16),
        ),
        in_specs=[vmem] * 9 + [hbm] * 3,
        out_specs=(vmem, vmem),
        scratch_shapes=[
            pltpu.VMEM((width, units), BF16),
            pltpu.VMEM((width, units), BF16),
            pltpu.VMEM((units, width), BF16),
            pltpu.VMEM((ep, cap, width), BF16),
            pltpu.VMEM((ep, tp_n, cap, width), BF16),
            pltpu.VMEM((ep, 2, cap, width), BF16),
            pltpu.VMEM((ep, cap, width), BF16),
            pltpu.VMEM((ep, cap, width), BF16),
            pltpu.VMEM((heads * span, dim), BF16),
            pltpu.VMEM((ep, 2 * span, dim), BF16),
            pltpu.VMEM((ep, heads, span), BF16),
            pltpu.VMEM((heads * span, dim), F32),
            pltpu.VMEM((heads * span, 128), F32),
            pltpu.VMEM((tp_n, share, width), BF16),
            pltpu.VMEM((2, share, width), BF16),
            pltpu.VMEM((share, width), BF16),
            dma((3,)),
        ] + [dma((ep,))] * 22 + [dma] * 6,
        compiler_params=pltpu.CompilerParams(
            collective_id=0, has_side_effects=True, vmem_limit_bytes=67043328
        ),
        cost_estimate=pl.CostEstimate(
            flops=6 * ep * tp_n * cap * width * units, bytes_accessed=6 * width * units,
            transcendentals=0,
        ),
        name="layer",
    )(
        jnp.transpose(routes), jnp.transpose(route_weights), tokens_b, moe_gain,
        queries,
        keys[:, 0], values[:, 0], jnp.transpose(key_bias), out_weight,
        gate_weight, up_weight, down_weight,
    )


def solution(mesh):
    in_specs = (
        P("ep", "tp", None),
        P("ep", "tp", None),
        P("ep", "tp", None),
        P("ep", "tp"),
        P("tp", None),
        P(("ep", "tp"), None),
        P(),
        P("ep", None, "tp"),
        P("ep", None, "tp"),
        P("ep", "tp", None),
        P(("ep", "tp"), None),
        P(("ep", "tp"), None),
    )
    out_specs = (P(("ep", "tp"), None), P(("ep", "tp"), None))
    return jax.shard_map(body, mesh=mesh, in_specs=in_specs, out_specs=out_specs, check_vma=False)
```

```python
import functools
import math

import jax
import jax.numpy as jnp
from jax import lax
from jax.experimental import pallas as pl
from jax.experimental.pallas import tpu as pltpu
from jax.sharding import PartitionSpec as P

MESH = pl.DeviceIdType.MESH
F32, BF16 = jnp.float32, jnp.bfloat16

SLOTS = 36
SENDS = ((6, 4, 3, 2, 1, 5, 7), (6, 1, 2, 5, 3, 7, 4))
PLAN = {
    'part': ((0, 6291568, 136331264, 5242880, 304, 0), (0, 458752, 72744992, 25165827, 0, 0)),
    'fin': ((0, 0, 460288, 262144, 50667648, 1), (0, 0, 28672, 329248, 25362496, 0)),
    'dot': ((2162688, 393223, 32832, 13568, 0, 0), (0, 38825984, 3163648, 32769, 0, 0)),
    'relay': ((67122977, 32774, 5, 0, 0, 0), (55005712, 1536, 8, 0, 0, 0)),
    'both': ((7348480, 58721856, 0, 5, 0, 0), (117440512, 101711954, 52, 2048, 0, 0)),
    'kvf': ((1048576, 512, 50331648, 64, 0, 0), (1, 0, 12320, 67108864, 0, 0)),
    'att': ((0, 1, 0, 70254594, 8848901, 0), (0, 65536, 0, 67305984, 34661, 0)),
    'mix1': ((0, 0, 0, 0, 1048576, 0), (0, 0, 0, 0, 65536, 0)),
    'mix2': ((0, 0, 0, 0, 1048576, 0), (0, 0, 0, 0, 65536, 0)),
}


def remote(src, dst, send_sem, recv_sem, **where):
    return pltpu.make_async_remote_copy(
        src_ref=src, dst_ref=dst, send_sem=send_sem, recv_sem=recv_sem,
        device_id=where, device_id_type=MESH,
    )


def dot(a, b):
    return jnp.dot(a, b, preferred_element_type=F32)


def flip(a, b, n):
    out, bit = 0, 1
    while bit < n:
        p, q = (a // bit) % 2, (b // bit) % 2
        out = out + bit * (p + q - 2 * p * q)
        bit *= 2
    return out


def columns(rows_ref):
    values = rows_ref[...].astype(F32)
    top, tok = values.shape
    return [
        jnp.transpose(jnp.broadcast_to(values[c : c + 1, :], (128, tok)))[:, 0:1] for c in range(top)
    ]


def slots_of(routes, me, ep, cap):
    tok, top = routes[0].shape[0], len(routes)
    lanes = max(128, -(-ep // 128) * 128)
    lane = lax.broadcasted_iota(jnp.int32, (tok, lanes), 1)
    picks = [(lane == routes[c]).astype(F32) for c in range(top)]
    named = functools.reduce(lambda a, b: a + b, picks)
    row = lax.broadcasted_iota(jnp.int32, (tok, tok), 0)
    col = lax.broadcasted_iota(jnp.int32, (tok, tok), 1)
    earlier = dot((col < row).astype(F32).astype(BF16), named.astype(BF16))
    places = []
    for c in range(top):
        slot = jnp.sum(earlier * picks[c], axis=1, keepdims=True).astype(jnp.int32)
        places.append((routes[c] ^ me) * cap + slot)
    return places


def moe_kernel(
    ep, tp_n, cap, heads,
    routes_ref, weights_ref, tokens_ref, gain_ref, q_ref, keys_ref, values_ref, bias_ref, wo_hbm,
    gate_hbm, up_hbm, down_hbm, mixed_ref, out_ref,
    wo_ref, gate, up, down, outbound, rows, core_in, x_in, ret,
    qs, kv, kb, acc, carried, part, mix_core, mix_x,
    w_sem, a_s, a_r, bx_s, bx_r, bc_s, bc_r, bd_s, bd_r,
    p0_s, p0_r, p1_s, p1_r, q_s, q_r, r_s, r_r,
    c_s, cb_s, m_s, mb_s, kv_r, kb_r,
    m0_s, m0_r, m1_s, m1_r, mq_s, mq_r,
):
    me, tp = lax.axis_index("ep"), lax.axis_index("tp")
    mate = tp + 1 - 2 * (tp % 2)
    across = (tp + 2) % 4
    mate_across = (mate + 2) % 4
    beside = me + 1 - 2 * (me % 2)
    place = ((me // 2 + 1) // 2) % 2
    span, dim = keys_ref.shape
    tok, width = tokens_ref.shape

    loads = [
        pltpu.make_async_copy(src, dst, w_sem.at[n])
        for n, (src, dst) in enumerate(
            ((gate_hbm.at[0], gate), (up_hbm.at[0], up), (down_hbm.at[0], down), (wo_hbm, wo_ref))
        )
    ]
    for load in loads:
        load.start()

    barrier = pltpu.get_barrier_semaphore()

    def greet(k, _):
        pl.semaphore_signal(barrier, inc=1, device_id={"ep": (me + k) % ep}, device_id_type=MESH)
        return 0

    lax.fori_loop(1, ep, greet, 0)
    for other in (mate, across):
        pl.semaphore_signal(barrier, inc=1, device_id={"tp": other}, device_id_type=MESH)

    kv[me, 0:span] = keys_ref[...]
    kv[me, span : 2 * span] = values_ref[...]
    kb[me] = bias_ref[...]
    wide = q_ref[...].astype(F32)
    for h in range(heads):
        qs[h * span : (h + 1) * span] = wide[:, h, :].astype(BF16)
    acc[...] = jnp.zeros_like(acc)
    carried[...] = jnp.zeros_like(carried)

    places = slots_of([c.astype(jnp.int32) for c in columns(routes_ref)], me, ep, cap)
    slot_id = lax.broadcasted_iota(jnp.int32, (tok, ep * cap), 1)
    hits = [(slot_id == place).astype(F32) for place in places]
    chosen = functools.reduce(lambda a, b: a + b, hits)
    tokens = tokens_ref[...].astype(F32)
    mean = jnp.mean(tokens * tokens, axis=1, keepdims=True)
    normed = (tokens * lax.rsqrt(mean + 1e-06) * gain_ref[...].astype(F32).reshape(1, width)).astype(BF16)
    packed = dot(jnp.transpose(chosen).astype(BF16), normed).astype(BF16)
    outbound[...] = packed.reshape(ep, cap, width)
    rows[0, tp] = packed[:cap]

    pl.semaphore_wait(barrier, ep + 1)

    planned = ep == 8

    def pick(choices, n):
        value = choices[-1]
        for c in range(len(choices) - 1):
            value = jnp.where(n == c, choices[c], value)
        return value

    def plan(i):
        if planned:
            word, digit = i // 7, 4 * (i % 7)
            work = {}
            for stage, table in PLAN.items():
                packed = pick([pick(row, place) for row in zip(*table)], word)
                entry = (packed >> digit) & 15
                work[stage] = (entry > 0, entry - 1)
            return work

        def lagged(lag):
            return (i >= lag) & (i < ep + lag), i - lag

        def turned(lag):
            active, p = lagged(lag)
            return active, jnp.where(p < ep - 2, p + 2, ep - 1 - p)

        return {
            "part": turned(5), "fin": turned(6), "dot": lagged(2), "relay": lagged(0),
            "both": lagged(1), "kvf": ((i == 0) | (i % 2 == 1), (i + 1) // 2), "att": lagged(2),
            "mix1": (i == ep + 2, 0), "mix2": (i == ep + 3, 0),
        }

    def dispatch(k):
        return remote(outbound.at[k], rows.at[k, tp], a_s.at[k], a_r.at[k], ep=flip(me, k, ep))

    def relay_across(k):
        return remote(rows.at[k, tp], rows.at[k, tp], bx_s.at[k], bx_r.at[k], tp=across)

    def relay_mate(k):
        return remote(rows.at[k, tp], rows.at[k, tp], bc_s.at[k], bc_r.at[k], tp=mate)

    def relay_both(k):
        return remote(rows.at[k, across], rows.at[k, across], bd_s.at[k], bd_r.at[k], tp=mate)

    def part_mate(k):
        return remote(rows.at[k, mate], core_in.at[k, 0], p0_s.at[k], p0_r.at[k], tp=mate)

    def part_mate_across(k):
        return remote(rows.at[k, mate_across], core_in.at[k, 1], p1_s.at[k], p1_r.at[k], tp=mate)

    def part_across(k):
        return remote(core_in.at[k, 1], x_in.at[k], q_s.at[k], q_r.at[k], tp=across)

    def give_back(k):
        return remote(x_in.at[k], ret.at[k], r_s.at[k], r_r.at[k], ep=flip(me, k, ep))

    def along(s):
        return (
            remote(kv.at[s], kv.at[s], c_s.at[s], kv_r.at[s], ep=(me + 2) % ep),
            remote(kb.at[s], kb.at[s], cb_s.at[s], kb_r.at[s], ep=(me + 2) % ep),
        )

    def aside(s):
        return (
            remote(kv.at[s], kv.at[s], m_s.at[s], kv_r.at[s], ep=beside),
            remote(kb.at[s], kb.at[s], mb_s.at[s], kb_r.at[s], ep=beside),
        )

    def pass_keys(j, act):
        s = me - 2 * j

        @pl.when((s >= 0) & (me + 2 < ep))
        def _():
            for copy in along(s):
                act(copy)

        @pl.when((s >= 0) & ((me % 2 == 0) | (j > 0)))
        def _():
            for copy in aside(s):
                act(copy)

    if planned:
        for turn in zip(*SENDS):
            dispatch(pick(turn, place)).start()
    else:
        def send(k, _):
            dispatch(k).start()
            return 0

        lax.fori_loop(1, ep, send, 0)

    mix_far = remote(part.at[mate_across], mix_core.at[1], m1_s, m1_r, tp=mate)
    mix_near = remote(part.at[mate], mix_core.at[0], m0_s, m0_r, tp=mate)
    mix_over = remote(mix_core.at[1], mix_x, mq_s, mq_r, tp=across)

    total_rows = heads * span
    nt = (((1,), (1,)), ((), ()))

    def attend(n):
        s = me - n
        key_no = lax.broadcasted_iota(jnp.int32, (total_rows, span), 1)
        query_no = lax.broadcasted_iota(jnp.int32, (total_rows, span), 0) % span
        tri = (
            lax.broadcasted_iota(jnp.int32, (span, span), 0)
            > lax.broadcasted_iota(jnp.int32, (span, span), 1)
        ).astype(F32).astype(BF16)
        bias = kb[s].astype(F32)
        scores = lax.dot_general(qs[...], kv[s, 0:span], nt, preferred_element_type=F32)
        scores = scores * (1.0 / math.sqrt(dim)) + jnp.concatenate(
            [jnp.broadcast_to(bias[h : h + 1, :], (span, span)) for h in range(heads)], axis=0
        )
        seen = (key_no < query_no) | (n > 0)
        soft = jnp.log(1.0 + jnp.exp(-jnp.abs(scores)))
        log_take = jnp.minimum(scores, 0.0) - soft
        log_keep = jnp.where(seen, log_take - scores, 0.0)
        high = log_keep.astype(BF16)
        low = (log_keep - high.astype(F32)).astype(BF16)
        after = dot(high, tri) + dot(low, tri)
        before = carried[:, 0:1]
        stick = jnp.where(seen, jnp.exp(log_take + after + before), 0.0).astype(BF16)
        acc[...] += dot(stick, kv[s, span : 2 * span])
        carried[...] = jnp.broadcast_to(
            before + jnp.sum(log_keep, axis=1, keepdims=True), carried.shape
        )

    def project():
        mixed = functools.reduce(
            lambda a, b: a + b,
            [
                dot(acc[h * span : (h + 1) * span].astype(BF16), wo_ref[h * dim : (h + 1) * dim, :])
                for h in range(heads)
            ],
        )
        part[...] = mixed.astype(BF16).reshape(part.shape)

    def step(i, _):
        work = plan(i)

        @pl.when(work["part"][0])
        def _():
            k = work["part"][1]
            part_mate(k).wait()
            part_mate_across(k).wait()
            core_in[k, 1] = (core_in[k, 1].astype(F32) + rows[k, across].astype(F32)).astype(BF16)
            part_across(k).start()

        @pl.when(work["fin"][0])
        def _():
            k = work["fin"][1]
            part_across(k).wait()
            total = (
                rows[k, tp].astype(F32) + core_in[k, 0].astype(F32) + x_in[k].astype(F32)
            ).astype(BF16)

            @pl.when(k > 0)
            def _():
                x_in[k] = total
                give_back(k).start()

            @pl.when(k == 0)
            def _():
                ret[0] = total

        @pl.when(work["dot"][0])
        def _():
            k = work["dot"][1]
            relay_mate(k).wait()
            relay_both(k).wait()
            relay_across(k).wait_send()
            x = rows[k].reshape(tp_n * cap, width)
            gated = dot(x, gate[...])
            lifted = dot(x, up[...])
            hidden = (gated / (1.0 + jnp.exp(-gated)) * lifted).astype(BF16)
            rows[k] = dot(hidden, down[...]).astype(BF16).reshape(tp_n, cap, width)
            part_mate(k).start()
            part_mate_across(k).start()

        @pl.when(work["relay"][0])
        def _():
            k = work["relay"][1]

            @pl.when(k > 0)
            def _():
                dispatch(k).wait_recv()

            relay_across(k).start()
            relay_mate(k).start()

        @pl.when(work["both"][0])
        def _():
            k = work["both"][1]
            relay_across(k).wait_recv()
            relay_both(k).start()

        @pl.when(work["kvf"][0] & (me - 2 * work["kvf"][1] >= 0))
        def _():
            j = work["kvf"][1]

            @pl.when(j > 0)
            def _():
                for copy in along(me - 2 * j):
                    copy.wait_recv()

            pass_keys(j, lambda copy: copy.start())

        @pl.when(work["att"][0] & (work["att"][1] <= me))
        def _():
            n = work["att"][1]

            @pl.when(n % 2 == 1)
            def _():
                for copy in aside(me - n):
                    copy.wait_recv()

            attend(n)

        @pl.when(work["mix1"][0])
        def _():
            project()
            mix_far.start()
            mix_near.start()

        @pl.when(work["mix2"][0])
        def _():
            mix_far.wait()
            mix_core[1] = (mix_core[1].astype(F32) + part[across].astype(F32)).astype(BF16)
            mix_over.start()

        return 0

    for load in loads:
        load.wait()
    lax.fori_loop(0, SLOTS if planned else ep + 6, step, 0)

    def drain(j, _):
        pass_keys(j, lambda copy: copy.wait_send())
        return 0

    lax.fori_loop(0, ep // 2, drain, 0)
    mix_near.wait()
    mix_over.wait()
    mixed_ref[...] = (
        part[tp].astype(F32) + mix_core[0].astype(F32) + mix_x[...].astype(F32)
    ).astype(BF16)

    def finish(k, _):
        dispatch(k).wait_send()
        give_back(k).wait()
        return 0

    lax.fori_loop(1, ep, finish, 0)
    weights = columns(weights_ref)
    mix = functools.reduce(
        lambda a, b: a + b, [hit * weights[c] for c, hit in enumerate(hits)]
    )
    high = mix.astype(BF16)
    low = (mix - high.astype(F32)).astype(BF16)
    results = ret[...].reshape(ep * cap, width)
    out_ref[...] = (dot(high, results) + dot(low, results)).astype(BF16)


def body(
    queries, keys, values, key_bias, out_weight, tokens_b, moe_gain,
    gate_weight, up_weight, down_weight, routes, route_weights,
):
    ep, tp_n = lax.axis_size("ep"), lax.axis_size("tp")
    tok, width = tokens_b.shape
    top = routes.shape[1]
    units = gate_weight.shape[2]
    experts = ep * gate_weight.shape[0]
    capacity = max(2, 3 * top * tok // (2 * experts))
    cap = -(-capacity // 16) * 16
    span, heads, dim = queries.shape
    share = span // tp_n
    vmem = pl.BlockSpec(memory_space=pltpu.VMEM)
    hbm = pl.BlockSpec(memory_space=pl.ANY)
    dma = pltpu.SemaphoreType.DMA
    return pl.pallas_call(
        functools.partial(moe_kernel, ep, tp_n, cap, heads),
        out_shape=(
            jax.ShapeDtypeStruct((share, width), BF16),
            jax.ShapeDtypeStruct((tok, width), BF16),
        ),
        in_specs=[vmem] * 8 + [hbm] * 4,
        out_specs=(vmem, vmem),
        scratch_shapes=[
            pltpu.VMEM((heads * dim, width), BF16),
            pltpu.VMEM((width, units), BF16),
            pltpu.VMEM((width, units), BF16),
            pltpu.VMEM((units, width), BF16),
            pltpu.VMEM((ep, cap, width), BF16),
            pltpu.VMEM((ep, tp_n, cap, width), BF16),
            pltpu.VMEM((ep, 2, cap, width), BF16),
            pltpu.VMEM((ep, cap, width), BF16),
            pltpu.VMEM((ep, cap, width), BF16),
            pltpu.VMEM((heads * span, dim), BF16),
            pltpu.VMEM((ep, 2 * span, dim), BF16),
            pltpu.VMEM((ep, heads, span), BF16),
            pltpu.VMEM((heads * span, dim), F32),
            pltpu.VMEM((heads * span, 128), F32),
            pltpu.VMEM((tp_n, share, width), BF16),
            pltpu.VMEM((2, share, width), BF16),
            pltpu.VMEM((share, width), BF16),
            dma((4,)),
        ] + [dma((ep,))] * 22 + [dma] * 6,
        compiler_params=pltpu.CompilerParams(
            collective_id=0, has_side_effects=True, vmem_limit_bytes=67043328
        ),
        cost_estimate=pl.CostEstimate(
            flops=6 * ep * tp_n * cap * width * units, bytes_accessed=6 * width * units,
            transcendentals=0,
        ),
        name="layer",
    )(
        jnp.transpose(routes), jnp.transpose(route_weights), tokens_b, moe_gain,
        queries,
        keys[:, 0], values[:, 0], jnp.transpose(key_bias), out_weight,
        gate_weight, up_weight, down_weight,
    )


def solution(mesh):
    in_specs = (
        P("ep", "tp", None),
        P("ep", "tp", None),
        P("ep", "tp", None),
        P("ep", "tp"),
        P("tp", None),
        P(("ep", "tp"), None),
        P(),
        P("ep", None, "tp"),
        P("ep", None, "tp"),
        P("ep", "tp", None),
        P(("ep", "tp"), None),
        P(("ep", "tp"), None),
    )
    out_specs = (P(("ep", "tp"), None), P(("ep", "tp"), None))
    return jax.shard_map(body, mesh=mesh, in_specs=in_specs, out_specs=out_specs, check_vma=False)
```
